32 devices in a mesh: grp: 2 (over y), kv: 4 (over z), tp: 4 (over x, core).
Axes of the slice: x: 2, y: 2, z: 4, core: 2. Of those that a mesh axis runs over, the one named last changes fastest.
Arguments:
- tokens: bfloat16 [4096, 2048], P(('grp', 'kv')), parts along dimension 0, may hold values from -72 to 72
- w_query: bfloat16 [2048, 1024], P(None, 'tp'), may hold values from -0.125 to 0.125
- w_key: bfloat16 [2048, 256], P(None, 'tp'), may hold values from -0.125 to 0.125
- w_value: bfloat16 [2048, 256], P(None, 'tp'), may hold values from -0.125 to 0.125
- w_out: bfloat16 [1024, 2048], P('tp'), may hold values from -0.1875 to 0.1875
- selection: int32 [4, 64, 32], P('tp', ('grp', 'kv')), parts along dimension 1, may hold values from -1 to 31, as said below
Outputs:
- attended_out: bfloat16 [4096, 2048], P(('grp', 'kv', 'tp')), parts along dimension 0
The draws below stay inside these ranges and needn't reach their ends.
There are 2 independent parts, one for each index of `grp`. The reference program is written for one: setup_inputs(seed, part) draws one part's arguments, and reference() takes and returns one part's arrays. A program takes and returns all parts, laid end to end along the dimension named above; an argument that names none is the same for every part. Nothing has to cross between parts.
Inputs may be any that keep to these rules, and one draw needn't show every extreme that they name: `selection`: entry 0 is the query block's own index; the others are distinct indices of earlier blocks, then -1 for unused entries. For one key head, the query blocks of one device's range together choose at most 2 distinct blocks of any other device's range, and some device reaches 2 in every draw.
All inputs are finite; a program needn't handle non-finite values.
Results may differ from the reference program's by a relative error of at most 0.028.
The reference program's roundings to bfloat16 on the way (of `queries`, `keys`, `values`, `weights` and `attended`) count: a program that leaves them out, or rounds other values in their place, can miss the bound.
Values may be sent and summed in bfloat16 or wider, within the bound.
A program may use at most 128 MiB of HBM per device.

```python
import jax
import jax.numpy as jnp
from jax import lax

D = 2048
HEADS = 16
KV_HEADS = 4
HEAD_DIM = 64
BLOCK = 64
TOPK = 32
CAP = 2
QB_DEV = 8
TOKENS = 2048
NQB = 32
N_TP = 4


def draw_tokens(key, part):
    normal_draw = jax.random.normal(jax.random.fold_in(key, 11), (TOKENS, D), jnp.float32)
    normal_draw = jnp.clip(normal_draw, -6.0, 6.0)
    return normal_draw.astype(jnp.bfloat16)


def draw_selection(key, part):
    per_dev = QB_DEV
    total_blocks = NQB
    devices = total_blocks // per_dev
    pair_score = jax.random.randint(jax.random.fold_in(key, 21), (KV_HEADS, devices, devices, per_dev), 0, 1 << 20) * per_dev + jnp.arange(per_dev)
    rank_in = jnp.sum((pair_score[..., None, :] > pair_score[..., :, None]).astype(jnp.int32), axis=-1)
    in_pair = rank_in < CAP
    popular = jax.random.randint(jax.random.fold_in(key, 22), (KV_HEADS, total_blocks), 0, 4) * 300
    noise_int = jax.random.randint(jax.random.fold_in(key, 23), (KV_HEADS, total_blocks, total_blocks), 0, 1000)
    block_ids = jnp.arange(total_blocks)
    owner_ids = block_ids // per_dev
    within_ids = block_ids % per_dev
    dev_of = block_ids // per_dev
    slot_of = block_ids % per_dev
    pair_here = in_pair[:, dev_of[:, None], owner_ids[None, :], within_ids[None, :]]
    remote = (owner_ids[None, :] < dev_of[:, None])[None] & pair_here
    earlier = (owner_ids[None, :] == dev_of[:, None]) & (within_ids[None, :] < slot_of[:, None])
    candidate = remote | earlier[None]
    forced = (owner_ids[None, :] == dev_of[:, None] - 1) & (slot_of == 1)[:, None] | (owner_ids[None, :] == dev_of[:, None] - devices // 2) & (slot_of == 2)[:, None]
    value_int = noise_int + popular[:, None, :] + 4096 * forced[None].astype(jnp.int32)
    score_int = jnp.where(candidate, value_int * total_blocks + block_ids, -1 - block_ids)
    top_scores, top_index = lax.top_k(score_int, TOPK - 1)
    others = jnp.where(top_scores >= 0, top_index, -1)
    own_block = jnp.broadcast_to(block_ids[None, :, None], (KV_HEADS, total_blocks, 1))
    return jnp.concatenate([own_block, others], axis=-1).astype(jnp.int32)


def level_of(key, extent, split, low, high):
    def one(axis_at, blocks):
        heights = jax.random.uniform(jax.random.fold_in(jax.random.fold_in(key, 6), axis_at), (blocks,), jnp.float32, low / len(split), high / len(split))
        return jnp.repeat(jnp.exp(heights), extent[axis_at] // blocks).reshape((-1,) + (1,) * (len(extent) - axis_at - 1))

    factor_of = one(*split[0])
    for cut in split[1:]:
        factor_of = factor_of * one(*cut)
    return factor_of


def noise(own_key, extent, deviation, bound, shards=(), kind=jnp.bfloat16):
    level = level_of(own_key, extent, shards, -0.22, 0.18) if shards else 1.0
    array = jax.random.normal(own_key, extent, jnp.float32) * deviation * level
    return jnp.minimum(jnp.maximum(array, -bound), bound).astype(kind)


def setup_inputs(seed: int = 0, part: int = 0) -> dict:
    splits = jax.random.split(jax.random.key(seed), 7)
    part_splits = jax.random.split(jax.random.fold_in(splits[6], part), 7)
    tokens = draw_tokens(jax.random.fold_in(jax.random.fold_in(splits[6], part), 71), part)
    w_query = noise(splits[1], (D, HEADS * HEAD_DIM), D ** -0.5, 0.125, ((1, 4),))
    w_key = noise(splits[2], (D, KV_HEADS * HEAD_DIM), D ** -0.5, 0.125, ((1, 4),))
    w_value = noise(splits[3], (D, KV_HEADS * HEAD_DIM), D ** -0.5, 0.125, ((1, 4),))
    w_out = noise(splits[4], (HEADS * HEAD_DIM, D), (HEADS * HEAD_DIM) ** -0.5, 0.1875, ((0, 4),))
    selection = draw_selection(jax.random.fold_in(jax.random.fold_in(splits[6], part), 71), part)
    return {"tokens": tokens, "w_query": w_query, "w_key": w_key, "w_value": w_value, "w_out": w_out, "selection": selection}


ROPE_BASE = 500000.0


def rotate(head_rows, positions):
    half = head_rows.shape[-1] // 2
    freqs = ROPE_BASE ** (-jnp.arange(half, dtype=jnp.float32) / half)
    angles = positions[:, None, None] * freqs
    cosine = jnp.cos(angles)
    sine = jnp.sin(angles)
    first = head_rows[..., :half]
    second = head_rows[..., half:]
    return jnp.concatenate([first * cosine - second * sine, second * cosine + first * sine], axis=-1)


def reference(tokens, w_query, w_key, w_value, w_out, selection):
    length = tokens.shape[0]
    positions = jnp.arange(length).astype(jnp.float32)
    queries = rotate(jnp.dot(tokens, w_query, preferred_element_type=jnp.float32).reshape(length, HEADS, HEAD_DIM), positions).astype(jnp.bfloat16)
    keys = rotate(jnp.dot(tokens, w_key, preferred_element_type=jnp.float32).reshape(length, KV_HEADS, HEAD_DIM), positions).astype(jnp.bfloat16)
    values = jnp.dot(tokens, w_value, preferred_element_type=jnp.float32).astype(jnp.bfloat16)
    key_blocks = jnp.transpose(keys.reshape(NQB, BLOCK, KV_HEADS, HEAD_DIM), (2, 0, 1, 3))
    value_blocks = jnp.transpose(values.reshape(NQB, BLOCK, KV_HEADS, HEAD_DIM), (2, 0, 1, 3))
    group = HEADS // KV_HEADS
    head_ids = jnp.arange(KV_HEADS)[:, None]
    offsets = jnp.arange(BLOCK).astype(jnp.int32)
    score_scale = HEAD_DIM ** -0.5

    def one_block(block_id):
        query_rows = lax.dynamic_slice_in_dim(queries, block_id * BLOCK, BLOCK, 0).reshape(BLOCK, KV_HEADS, group, HEAD_DIM)
        chosen_ids = lax.dynamic_index_in_dim(selection, block_id, 1, keepdims=False)
        safe_ids = jnp.maximum(chosen_ids, 0)
        picked_keys = key_blocks[head_ids, safe_ids].reshape(KV_HEADS, TOPK * BLOCK, HEAD_DIM)
        picked_values = value_blocks[head_ids, safe_ids].reshape(KV_HEADS, TOPK * BLOCK, HEAD_DIM)
        scores = jnp.einsum('qhgd,hkd->hgqk', query_rows.astype(jnp.float32), picked_keys.astype(jnp.float32)) * score_scale
        key_pos = (chosen_ids[:, :, None] * BLOCK + offsets).reshape(KV_HEADS, TOPK * BLOCK)
        live_keys = jnp.repeat(chosen_ids >= 0, BLOCK, axis=1)
        query_pos = block_id * BLOCK + offsets
        allowed = live_keys[:, None, None, :] & (key_pos[:, None, None, :] <= query_pos[None, None, :, None])
        scores = jnp.where(allowed, scores, -jnp.inf)
        top_score = jnp.max(scores, axis=-1, keepdims=True)
        expo = jnp.exp(scores - top_score)
        weights = (expo / jnp.sum(expo, axis=-1, keepdims=True)).astype(jnp.bfloat16)
        attended = jnp.einsum('hgqk,hkd->qhgd', weights.astype(jnp.float32), picked_values.astype(jnp.float32)).astype(jnp.bfloat16)
        return attended.reshape(BLOCK, HEADS * HEAD_DIM)

    attended = lax.map(one_block, jnp.arange(NQB).astype(jnp.int32)).reshape(length, HEADS * HEAD_DIM)
    width = HEADS * HEAD_DIM // N_TP
    summed = jnp.zeros((length, D), jnp.float32)
    for group_id in range(N_TP):
        partial_out = jnp.dot(attended[:, group_id * width:(group_id + 1) * width], w_out[group_id * width:(group_id + 1) * width], preferred_element_type=jnp.float32).astype(jnp.bfloat16)
        summed = summed + lax.optimization_barrier(partial_out).astype(jnp.float32)
    return summed.astype(jnp.bfloat16)
```

```python
import functools

import jax
import jax.numpy as jnp
import numpy as np
from jax import lax
from jax.experimental import pallas as pl
from jax.experimental.pallas import tpu as pltpu
from jax.sharding import PartitionSpec as P

HEAD_DIM = 64
BLOCK = 64
ROPE_BASE = 500000.0
NEG = -1e30
CUTS = (0, 1, 2, 4, 6, 8)
LATE = ((0, 1), (2,), (3,), (4,))
TOK_PARTS = 4
MESH = pl.DeviceIdType.MESH
NT = (((1,), (1,)), ((), ()))


def tables(n_blocks):
    half = HEAD_DIM // 2
    lane = np.arange(128)
    freqs = ROPE_BASE ** (-(lane % half).astype(np.float64) / half)
    sign = np.where(lane % HEAD_DIM < half, -1.0, 1.0)
    inner = np.arange(BLOCK)[:, None] * freqs
    outer = (np.arange(n_blocks) * BLOCK)[:, None] * freqs
    inside = [np.cos(inner), np.sin(inner), sign * np.cos(inner), sign * np.sin(inner)]
    return np.concatenate(inside + [np.cos(outer), np.sin(outer)]).astype(np.float32)


def kernel(
    n, n_tp, n_grp,
    tok_h, wq_h, wk_h, wv_h, wo_h, sel_h, tab_h,
    o_ref,
    tab, tok, wq, w_kv, wfull, sel_all, qf, kv_own, send_kv, recv_kv,
    bias_l, bias_r, acc_s, max_s, qs_s, att, att_in, total_s,
    in_sem, sel_ss, sel_rs, kv_ss, kv_rs, w_ss, x_rs, l_rs, own_rs, near_rs, a_ss, a_rs,
):
    grp = lax.axis_index("grp")
    me = lax.axis_index("kv")
    t = lax.axis_index("tp")
    rows = tok.shape[0]
    blocks = rows // BLOCK
    heads = wq.shape[1] // HEAD_DIM
    topk = sel_all.shape[2]
    group_rows = heads * BLOCK
    far = lax.rem(t + n_tp // 2, n_tp)
    near = t + 1 - 2 * lax.rem(t, 2)
    other = n_grp - 1 - grp
    width = wo_h.shape[0]
    side = lax.rem(me, 2)
    beside = me + 1 - 2 * side
    mine, from_y, from_z, last_part = grp * 2 + side, other * 2 + side, grp * 2 + 1 - side, other * 2 + 1 - side
    quarter = width // (2 * n_grp)
    unit = quarter // CUTS[-1]
    tok_rows = rows // TOK_PARTS
    late_of = [k for k, group in enumerate(LATE) for c in group]

    def local(src, dst, k):
        return pltpu.make_async_copy(src, dst, in_sem.at[k])

    def part_rows(part_of, lo=0, hi=CUTS[-1]):
        return pl.ds(part_of * quarter + lo * unit, (hi - lo) * unit)

    def w_load(part_of, k):
        return local(wo_h.at[part_rows(part_of)], wfull.at[t, part_rows(part_of)], k)

    sel_load = local(sel_h.at[0], sel_all.at[me], 0)
    w_first, w_second = w_load(mine, 1), w_load(last_part, 2)
    kv_loads = [
        local(wk_h, w_kv.at[:HEAD_DIM], 3), local(wv_h, w_kv.at[HEAD_DIM:], 3), local(tab_h, tab, 5 + TOK_PARTS),
    ]
    tok_loads = []
    for k in range(TOK_PARTS):
        part = pl.ds(k * tok_rows, tok_rows)
        tok_loads.append(local(tok_h.at[part], tok.at[part], 5 + k))
    q_load = local(wq_h, wq, 4)
    w_rest = [w_load(from_y, 1), w_load(from_z, 1)]
    for load in [sel_load, w_first, *kv_loads, tok_loads[0], w_second, *tok_loads[1:], q_load]:
        load.start()

    barrier = pltpu.get_barrier_semaphore()
    for k in range(1, n_tp):
        pl.semaphore_signal(barrier, inc=1, device_id={"tp": lax.rem(t + k, n_tp)}, device_id_type=MESH)
    for k in range(1, n_grp):
        pl.semaphore_signal(barrier, inc=1, device_id={"grp": lax.rem(grp + k, n_grp)}, device_id_type=MESH)
    for r in range(1, n):
        @pl.when(r > me)
        def _():
            pl.semaphore_signal(barrier, inc=1, device_id={"kv": r}, device_id_type=MESH)

    @pl.when(side == 1)
    def _():
        pl.semaphore_signal(barrier, inc=1, device_id={"kv": beside}, device_id_type=MESH)

    def remote(src, dst, ss, rs, axis, index):
        return pltpu.make_async_remote_copy(
            src_ref=src, dst_ref=dst, send_sem=ss, recv_sem=rs,
            device_id={axis: index}, device_id_type=MESH,
        )

    def x_copy(c, owner):
        at = part_rows(mine, CUTS[c], CUTS[c + 1])
        return remote(wfull.at[owner, at], wfull.at[owner, at], w_ss, x_rs.at[c], "tp", far)

    def x_last(owner):
        at = part_rows(last_part, CUTS[-1] // 2)
        return remote(wfull.at[owner, at], wfull.at[owner, at], w_ss, x_rs.at[len(CUTS) - 1], "tp", far)

    def link_copy(axis, to, part_of, lo, hi, k):
        at = wfull.at[far, part_rows(part_of, lo, hi)]
        return remote(at, at, w_ss, l_rs.at[k], axis, to)

    def y_copy(c, part_of, k):
        return link_copy("grp", other, part_of, CUTS[c], CUTS[c + 1], k)

    def z_copy(c, part_of, k):
        return link_copy("kv", beside, part_of, CUTS[c], CUTS[c + 1], k)

    def y_last(part_of):
        return link_copy("grp", other, part_of, 0, CUTS[-1] // 4, len(LATE))

    def z_last(part_of):
        return link_copy("kv", beside, part_of, CUTS[-1] // 4, CUTS[-1] // 2, len(LATE))

    def near_copy(part_of, lo, hi):
        at = wfull.at[far, part_rows(part_of, lo, hi)]
        return remote(at, at, w_ss, near_rs, "tp", near)

    def own_copy(owner):
        return remote(wfull.at[owner], wfull.at[owner], w_ss, own_rs, "tp", near)

    def sel_copy(source, to):
        return remote(sel_all.at[source], sel_all.at[source], sel_ss, sel_rs.at[source], "kv", to)

    def kv_copy(source, to):
        return remote(send_kv.at[to], recv_kv.at[source], kv_ss, kv_rs.at[source], "kv", to)

    def pass_on(c):
        x_copy(c, far).wait_recv()
        y_copy(c, mine, late_of[c]).start()
        z_copy(c, mine, late_of[c]).start()
        near_copy(mine, CUTS[c], CUTS[c + 1]).start()

    def pass_late(k):
        lo, hi = CUTS[LATE[k][0]], CUTS[LATE[k][-1] + 1]
        link_copy("grp", other, 0, 0, 2 * (hi - lo), k).wait_recv()
        if k == 0:
            y_last(from_z).start()
        if k == 1:
            z_last(from_y).start()
        near_copy(from_y, lo, hi).start()
        near_copy(from_z, lo, hi).start()

    def pass_x_last():
        x_last(far).wait_recv()
        near_copy(last_part, CUTS[-1] // 2, CUTS[-1]).start()

    def pass_last():
        link_copy("grp", other, 0, 0, CUTS[-1] // 2, len(LATE)).wait_recv()
        near_copy(last_part, 0, CUTS[-1] // 2).start()

    sel_load.wait()
    w_first.wait()
    pl.semaphore_wait(barrier, n_tp + n_grp - 2 + me + 1 - side)
    for c in range(len(CUTS) - 1):
        x_copy(c, t).start()
    for s in range(n - 1):
        @pl.when(s < me)
        def _():
            sel_copy(me, s).start()
    w_second.wait()
    x_last(t).start()
    for load in w_rest:
        load.start()

    for s in range(n - 1):
        @pl.when(s >= me)
        def _():
            recv_kv[s] = jnp.zeros(recv_kv.shape[1:], recv_kv.dtype)

    lane = lax.broadcasted_iota(jnp.int32, (BLOCK, 128), 1)
    low = lane < HEAD_DIM
    first = lax.rem(lane, HEAD_DIM) < HEAD_DIM // 2

    def angle(i):
        at = 4 * BLOCK + me * blocks + i
        cos_b = tab[pl.ds(at, 1), :]
        sin_b = tab[pl.ds(at + n * blocks, 1), :]
        cos_i, sin_i, cos_s, sin_s = (tab[k * BLOCK:(k + 1) * BLOCK, :] for k in range(4))
        return cos_i * cos_b - sin_i * sin_b, sin_s * cos_b + cos_s * sin_b

    def rotated(x, cos, sin):
        swapped = jnp.where(first, pltpu.roll(x, 96, 1), pltpu.roll(x, 32, 1))
        return x * cos + swapped * sin

    local(w_kv, w_kv, 3).wait()
    kv_loads[2].wait()
    per_part = tok_rows // BLOCK
    for i in range(blocks):
        if i % per_part == 0:
            tok_loads[i // per_part].wait()
            at = i * BLOCK
            qf[at:at + tok_rows, :128] = lax.dot_general(
                tok[at:at + tok_rows, :], w_kv[...], NT, preferred_element_type=jnp.float32
            )
        cos, sin = angle(i)
        x = qf[i * BLOCK:(i + 1) * BLOCK, :128]
        turned = rotated(x, jnp.where(low, cos, 1.0), jnp.where(low, sin, 0.0))
        kv_own[i * BLOCK:(i + 1) * BLOCK, :] = turned.astype(jnp.bfloat16)

    def ends(sel, source):
        e = sel - source * blocks
        inside = (e >= 0) & (e < blocks)
        ef = e.astype(jnp.float32)
        lo = jnp.where(inside, ef, 1e6)
        hi = jnp.where(inside, ef, -1e6)
        lo = jnp.min(jnp.min(lo, axis=1, keepdims=True), axis=0, keepdims=True)
        hi = jnp.max(jnp.max(hi, axis=1, keepdims=True), axis=0, keepdims=True)
        return lo, hi

    r_iota = lax.broadcasted_iota(jnp.int32, (2 * BLOCK, rows), 0)
    c_iota = lax.broadcasted_iota(jnp.int32, (2 * BLOCK, rows), 1)
    r_in = lax.rem(r_iota, BLOCK).astype(jnp.float32)
    c_f = c_iota.astype(jnp.float32)
    for r in range(n - 1, 0, -1):
        @pl.when(r > me)
        def _():
            sel_copy(r, r).wait_recv()
            lo, hi = ends(sel_all[r], me)
            want = jnp.where(r_iota < BLOCK, lo, hi) * BLOCK + r_in
            pick = jnp.where(c_f == want, 1.0, 0.0).astype(jnp.bfloat16)
            chosen = jnp.dot(pick, kv_own[...], preferred_element_type=jnp.float32)
            send_kv[r] = chosen.astype(jnp.bfloat16)
            kv_copy(me, r).start()

    both = pl.ds(0, 2 * quarter)
    local(wo_h.at[both], wfull.at[t, both], 1).wait()
    own_copy(t).start()
    pass_on(0)

    q_load.wait()
    qf[...] = jnp.dot(tok[...], wq[...], preferred_element_type=jnp.float32)

    pass_on(1)
    sel_f = sel_all[me].astype(jnp.float32)
    base = (me * blocks).astype(jnp.float32)
    local_id = (lax.broadcasted_iota(jnp.int32, (blocks, rows), 1) // BLOCK).astype(jnp.float32) + base
    hit = jnp.zeros((blocks, rows), jnp.float32)
    for k in range(topk):
        hit = jnp.where(sel_f[:, k:k + 1] == local_id, 1.0, hit)
    bias_l[...] = jnp.where(hit > 0.5, 0.0, NEG)

    slot = lax.broadcasted_iota(jnp.int32, (blocks, 2 * BLOCK), 1)
    for s in range(n - 1):
        lo, hi = ends(sel_all[me], s)
        ident = jnp.where(slot < BLOCK, lo, jnp.where(hi != lo, hi, -1e6)) + (s * blocks)
        hit = jnp.zeros((blocks, 2 * BLOCK), jnp.float32)
        for k in range(topk):
            hit = jnp.where(sel_f[:, k:k + 1] == ident, 1.0, hit)
        bias_r[s] = jnp.where((hit > 0.5) & (s < me), 0.0, NEG)

    def with_ones(kv):
        at = lax.broadcasted_iota(jnp.int32, kv.shape, 1)
        return jnp.where(at < HEAD_DIM, jnp.ones_like(kv), kv)

    q_row = lax.rem(lax.broadcasted_iota(jnp.int32, (group_rows, 128), 0), BLOCK)
    q_col = lax.broadcasted_iota(jnp.int32, (group_rows, 128), 1)
    zero = jnp.zeros((BLOCK, 128), jnp.float32)

    for i in range(blocks):
        cos, sin = angle(i)
        cos, sin = cos * HEAD_DIM ** -0.5, sin * HEAD_DIM ** -0.5
        stacked = []
        for pair in range(heads // 2):
            turned = rotated(qf[i * BLOCK:(i + 1) * BLOCK, pair * 128:(pair + 1) * 128], cos, sin)
            stacked.append(jnp.where(low, turned, zero))
            stacked.append(jnp.where(low, pltpu.roll(turned, HEAD_DIM, 1), zero))
        qs = jnp.concatenate(stacked, axis=0).astype(jnp.bfloat16)
        qs_s[i] = qs
        keys = 128 * (i // 2 + 1)
        kv = kv_own[:keys, :]
        scores = lax.dot_general(qs, kv, NT, preferred_element_type=jnp.float32)
        scores = scores + bias_l[i:i + 1, :keys]
        last = jnp.where(q_col <= q_row + (i % 2) * BLOCK, scores[:, keys - 128:], NEG)
        scores = last if keys == 128 else jnp.concatenate([scores[:, :keys - 128], last], axis=1)
        top = jnp.max(scores, axis=1, keepdims=True)
        p = jnp.exp(scores - top).astype(jnp.bfloat16)
        acc_s[i] = jnp.dot(p, with_ones(kv), preferred_element_type=jnp.float32)
        max_s[i] = jnp.broadcast_to(top, (group_rows, 128))
        if i == blocks // 4:
            pass_on(2)
        if i == blocks // 2 + 1:
            pass_on(3)
    pass_late(0)

    for s in range(n - 1):
        @pl.when(s < me)
        def _():
            kv_copy(s, s).wait_recv()

    step = max(k for k in (1, 2, 3, 4) if (n - 1) % k == 0)

    def remote_part(at, i):
        kv = recv_kv[pl.ds(at * step, step)].reshape(step * 128, 128)
        scores = lax.dot_general(qs_s[i], kv, NT, preferred_element_type=jnp.float32)
        scores = jnp.concatenate(
            [scores[:, k * 128:(k + 1) * 128] + bias_r[at * step + k, pl.ds(i, 1), :] for k in range(step)], axis=1
        )
        before = max_s[i]
        top = jnp.maximum(before[:, :1], jnp.max(scores, axis=1, keepdims=True))
        p = jnp.exp(scores - top).astype(jnp.bfloat16)
        acc_s[i] = acc_s[i] * jnp.exp(before - top) + jnp.dot(
            p, with_ones(kv), preferred_element_type=jnp.float32
        )
        if n - 1 > step:
            max_s[i] = jnp.broadcast_to(top, (group_rows, 128))

    per = blocks // n_tp

    def att_copy(owner, to, k):
        return remote(att.at[to], att_in.at[owner], a_ss, a_rs.at[k], "tp", to)

    far_near = lax.rem(near + n_tp // 2, n_tp)
    for turn, d in enumerate((far, far_near, near, t)):
        for b in range(per):
            i = d * per + b

            @pl.when(me > 0)
            def _():
                if n - 1 > step:
                    lax.fori_loop(0, (n - 1) // step, lambda at, _: (remote_part(at, i), 0)[1], 0)
                else:
                    remote_part(0, i)

            for pair in range(heads // 2):
                even = acc_s[i, (2 * pair) * BLOCK:(2 * pair + 1) * BLOCK, :]
                odd = acc_s[i, (2 * pair + 1) * BLOCK:(2 * pair + 2) * BLOCK, :]
                top = jnp.where(low, pltpu.roll(even, HEAD_DIM, 1), odd)
                bottom = jnp.where(low, even, pltpu.roll(odd, HEAD_DIM, 1))
                att[d, b * BLOCK:(b + 1) * BLOCK, pair * 128:(pair + 1) * 128] = (top / bottom).astype(jnp.bfloat16)
        if turn < n_tp - 1:
            att_copy(t, d, turn // 2).start()
        if turn == 0:
            pass_on(4)
        if turn < len(LATE) - 1:
            pass_late(turn + 1)
        if turn == 2:
            pass_x_last()

    pass_last()
    own_copy(near).wait_recv()
    att_copy(near, near, 1).wait_recv()
    span = 512
    spans = [slice(col, col + span) for col in range(0, o_ref.shape[1], span)]
    for cols in spans:
        total = jnp.dot(att[t], wfull[t, :, cols], preferred_element_type=jnp.float32)
        total_s[:, cols] = total + jnp.dot(att_in[near], wfull[near, :, cols], preferred_element_type=jnp.float32)

    remote(wfull.at[far_near], wfull.at[far_near], w_ss, near_rs, "tp", near).wait_recv()
    remote(att_in.at[:2], att_in.at[:2], a_ss, a_rs.at[0], "tp", near).wait_recv()
    for cols in spans:
        total = total_s[:, cols] + jnp.dot(att_in[far], wfull[far, :, cols], preferred_element_type=jnp.float32)
        total += jnp.dot(att_in[far_near], wfull[far_near, :, cols], preferred_element_type=jnp.float32)
        o_ref[:, cols] = total.astype(jnp.bfloat16)

    remote(wfull.at[:3], wfull.at[:3], w_ss, near_rs, "tp", near).wait_send()
    remote(att.at[:3], att.at[:3], a_ss, near_rs, "tp", near).wait_send()
    for k in range(1, n):
        @pl.when(me == k)
        def _():
            remote(sel_all.at[:k], sel_all.at[:k], sel_ss, sel_rs.at[0], "kv", beside).wait_send()

        @pl.when(me == n - 1 - k)
        def _():
            remote(send_kv.at[:k], send_kv.at[:k], kv_ss, kv_rs.at[0], "kv", beside).wait_send()


def solution(mesh):
    n, n_tp, n_grp = mesh.shape["kv"], mesh.shape["tp"], mesh.shape["grp"]
    assert n_tp == 4 and n_grp == 2 and n % 2 == 0

    def shards(tokens, w_query, w_key, w_value, w_out, selection):
        rows, depth = tokens.shape
        q_width, width = w_query.shape[1], w_out.shape[1]
        blocks, topk = selection.shape[1:]
        heads = q_width // HEAD_DIM
        table = tables(n * blocks)
        bf, f32 = jnp.bfloat16, jnp.float32
        hbm = pl.BlockSpec(memory_space=pl.ANY)
        vmem = pl.BlockSpec(memory_space=pltpu.VMEM)
        dma = pltpu.SemaphoreType.DMA
        out_rows = rows // n_tp
        return pl.pallas_call(
            functools.partial(kernel, n, n_tp, n_grp),
            out_shape=pltpu.VMEM((out_rows, width), bf),
            in_specs=[hbm] * 7,
            out_specs=vmem,
            scratch_shapes=[
                pltpu.VMEM(table.shape, f32),
                pltpu.VMEM((rows, depth), bf),
                pltpu.VMEM((depth, q_width), bf),
                pltpu.VMEM((2 * HEAD_DIM, depth), bf),
                pltpu.VMEM((n_tp, q_width, width), bf),
                pltpu.VMEM((n, blocks, topk), jnp.int32),
                pltpu.VMEM((rows, q_width), f32),
                pltpu.VMEM((rows, 128), bf),
                pltpu.VMEM((n, 128, 128), bf),
                pltpu.VMEM((n - 1, 128, 128), bf),
                pltpu.VMEM((blocks, rows), f32),
                pltpu.VMEM((n - 1, blocks, 128), f32),
                pltpu.VMEM((blocks, heads * BLOCK, 128), f32),
                pltpu.VMEM((blocks, heads * BLOCK, 128), f32),
                pltpu.VMEM((blocks, heads * BLOCK, 128), bf),
                pltpu.VMEM((n_tp, out_rows, q_width), bf),
                pltpu.VMEM((n_tp, out_rows, q_width), bf),
                pltpu.VMEM((out_rows, width), f32),
                dma((6 + TOK_PARTS,)),
                dma, dma((n,)), dma, dma((n - 1,)),
                dma, dma((len(CUTS),)), dma((len(LATE) + 1,)), dma, dma, dma, dma((2,)),
            ],
            compiler_params=pltpu.CompilerParams(
                collective_id=0, has_side_effects=True, vmem_limit_bytes=60 * 1024 * 1024
            ),
        )(tokens, w_query, w_key.T, w_value.T, w_out, selection, table)

    placed = (
        P(("grp", "kv"), None),
        P(None, "tp"),
        P(None, "tp"),
        P(None, "tp"),
        P("tp", None),
        P("tp", ("grp", "kv"), None),
    )
    return jax.shard_map(
        shards, mesh=mesh, in_specs=placed, out_specs=P(("grp", "kv", "tp"), None), check_vma=False
    )
```

```python
import functools

import jax
import jax.numpy as jnp
import numpy as np
from jax import lax
from jax.experimental import pallas as pl
from jax.experimental.pallas import tpu as pltpu
from jax.sharding import PartitionSpec as P

HEAD_DIM = 64
BLOCK = 64
ROPE_BASE = 500000.0
NEG = -1e30
CUTS = (0, 1, 2, 4, 6, 8)
LATE = ((0, 1), (2,), (3,), (4,))
TOK_PARTS = 2
ON, ANSWER = 0, 1
STEPS = {2: ((ANSWER, 1), (ON, 0), (ON, 1)), 3: ((ANSWER, 2),), 4: ((ANSWER, 3), (ON, 2)), 6: ((ON, 3),)}
MESH = pl.DeviceIdType.MESH
NT = (((1,), (1,)), ((), ()))


def tables(n_blocks):
    half = HEAD_DIM // 2
    lane = np.arange(128)
    freqs = ROPE_BASE ** (-(lane % half).astype(np.float64) / half)
    sign = np.where(lane % HEAD_DIM < half, -1.0, 1.0)
    inner = np.arange(BLOCK)[:, None] * freqs
    outer = (np.arange(n_blocks) * BLOCK)[:, None] * freqs
    inside = [np.cos(inner), np.sin(inner), sign * np.cos(inner), sign * np.sin(inner)]
    return np.concatenate(inside + [np.cos(outer), np.sin(outer)]).astype(np.float32)


def kernel(
    n, n_tp, n_grp,
    tok_h, wq_h, wk_h, wv_h, wo_h, sel_h, tab_h,
    o_ref,
    tab, tok, w_qkv, w_kv, wfull, sel_all, qf, kv_own, send_kv, recv_kv,
    bias_l, bias_r, acc_s, max_s, qs_s, att, att_in, total_s,
    in_sem, sel_ss, sel_rs, kv_ss, kv_rs, w_ss, x_rs, l_rs, own_rs, near_rs, a_ss, a_rs,
):
    grp = lax.axis_index("grp")
    me = lax.axis_index("kv")
    t = lax.axis_index("tp")
    rows = tok.shape[0]
    blocks = rows // BLOCK
    q_width = wq_h.shape[1]
    heads = q_width // HEAD_DIM
    topk = sel_all.shape[2]
    group_rows = heads * BLOCK
    far = lax.rem(t + n_tp // 2, n_tp)
    near = t + 1 - 2 * lax.rem(t, 2)
    other = n_grp - 1 - grp
    width = wo_h.shape[0]
    side = lax.rem(me, 2)
    beside = me + 1 - 2 * side
    mine, from_y, from_z, last_part = grp * 2 + side, other * 2 + side, grp * 2 + 1 - side, other * 2 + 1 - side
    quarter = width // (2 * n_grp)
    unit = quarter // CUTS[-1]
    tok_rows = rows // TOK_PARTS
    late_of = [k for k, group in enumerate(LATE) for c in group]

    def local(src, dst, k):
        return pltpu.make_async_copy(src, dst, in_sem.at[k])

    def part_rows(part_of, lo=0, hi=CUTS[-1]):
        return pl.ds(part_of * quarter + lo * unit, (hi - lo) * unit)

    def w_load(part_of, k):
        return local(wo_h.at[part_rows(part_of)], wfull.at[t, part_rows(part_of)], k)

    sel_load = local(sel_h.at[0], sel_all.at[me], 0)
    w_first, w_second = w_load(mine, 1), w_load(last_part, 2)
    kv_loads = [
        local(wk_h, w_kv.at[:HEAD_DIM], 3), local(wv_h, w_kv.at[HEAD_DIM:], 3), local(tab_h, tab, 5 + TOK_PARTS),
    ]
    tok_loads = []
    for k in range(TOK_PARTS):
        part = pl.ds(k * tok_rows, tok_rows)
        tok_loads.append(local(tok_h.at[part], tok.at[part], 5 + k))
    q_load = local(wq_h, w_qkv.at[:, :q_width], 4)
    w_rest = [w_load(from_y, 1), w_load(from_z, 1)]
    for load in [sel_load, w_first, *kv_loads, q_load, tok_loads[0], w_second, *tok_loads[1:]]:
        load.start()

    barrier = pltpu.get_barrier_semaphore()
    for k in range(1, n_tp):
        pl.semaphore_signal(barrier, inc=1, device_id={"tp": lax.rem(t + k, n_tp)}, device_id_type=MESH)
    for k in range(1, n_grp):
        pl.semaphore_signal(barrier, inc=1, device_id={"grp": lax.rem(grp + k, n_grp)}, device_id_type=MESH)
    for r in range(1, n):
        @pl.when(r > me)
        def _():
            pl.semaphore_signal(barrier, inc=1, device_id={"kv": r}, device_id_type=MESH)

    @pl.when(side == 1)
    def _():
        pl.semaphore_signal(barrier, inc=1, device_id={"kv": beside}, device_id_type=MESH)

    def remote(src, dst, ss, rs, axis, index):
        return pltpu.make_async_remote_copy(
            src_ref=src, dst_ref=dst, send_sem=ss, recv_sem=rs,
            device_id={axis: index}, device_id_type=MESH,
        )

    def x_copy(c, owner):
        at = part_rows(mine, CUTS[c], CUTS[c + 1])
        return remote(wfull.at[owner, at], wfull.at[owner, at], w_ss, x_rs.at[c], "tp", far)

    def x_last(owner):
        at = part_rows(last_part, CUTS[-1] // 2)
        return remote(wfull.at[owner, at], wfull.at[owner, at], w_ss, x_rs.at[len(CUTS) - 1], "tp", far)

    def link_copy(axis, to, part_of, lo, hi, k):
        at = wfull.at[far, part_rows(part_of, lo, hi)]
        return remote(at, at, w_ss, l_rs.at[k], axis, to)

    def y_copy(c, part_of, k):
        return link_copy("grp", other, part_of, CUTS[c], CUTS[c + 1], k)

    def z_copy(c, part_of, k):
        return link_copy("kv", beside, part_of, CUTS[c], CUTS[c + 1], k)

    def y_last(part_of):
        return link_copy("grp", other, part_of, 0, CUTS[-1] // 4, len(LATE))

    def z_last(part_of):
        return link_copy("kv", beside, part_of, CUTS[-1] // 4, CUTS[-1] // 2, len(LATE))

    def near_copy(part_of, lo, hi):
        at = wfull.at[far, part_rows(part_of, lo, hi)]
        return remote(at, at, w_ss, near_rs, "tp", near)

    def own_copy(owner):
        return remote(wfull.at[owner], wfull.at[owner], w_ss, own_rs, "tp", near)

    def sel_copy(source, to):
        return remote(sel_all.at[source], sel_all.at[source], sel_ss, sel_rs.at[source], "kv", to)

    def kv_copy(source, to):
        return remote(send_kv.at[to], recv_kv.at[source], kv_ss, kv_rs.at[source], "kv", to)

    def pass_on(c):
        x_copy(c, far).wait_recv()
        y_copy(c, mine, late_of[c]).start()
        z_copy(c, mine, late_of[c]).start()
        near_copy(mine, CUTS[c], CUTS[c + 1]).start()

    def pass_late(k):
        lo, hi = CUTS[LATE[k][0]], CUTS[LATE[k][-1] + 1]
        link_copy("grp", other, 0, 0, 2 * (hi - lo), k).wait_recv()
        if k == 0:
            y_last(from_z).start()
        if k == 1:
            z_last(from_y).start()
        near_copy(from_y, lo, hi).start()
        near_copy(from_z, lo, hi).start()

    def pass_x_last():
        x_last(far).wait_recv()
        near_copy(last_part, CUTS[-1] // 2, CUTS[-1]).start()

    def pass_last():
        link_copy("grp", other, 0, 0, CUTS[-1] // 2, len(LATE)).wait_recv()
        near_copy(last_part, 0, CUTS[-1] // 2).start()

    sel_load.wait()
    w_first.wait()
    pl.semaphore_wait(barrier, n_tp + n_grp - 2 + me + 1 - side)
    for c in range(len(CUTS) - 1):
        x_copy(c, t).start()
    for s in range(n - 1):
        @pl.when(s < me)
        def _():
            sel_copy(me, s).start()

    for s in range(n - 1):
        @pl.when(s >= me)
        def _():
            recv_kv[s] = jnp.zeros(recv_kv.shape[1:], recv_kv.dtype)

    lane = lax.broadcasted_iota(jnp.int32, (BLOCK, 128), 1)
    low = lane < HEAD_DIM
    first = lax.rem(lane, HEAD_DIM) < HEAD_DIM // 2

    def angle(i):
        at = 4 * BLOCK + me * blocks + i
        cos_b = tab[pl.ds(at, 1), :]
        sin_b = tab[pl.ds(at + n * blocks, 1), :]
        cos_i, sin_i, cos_s, sin_s = (tab[k * BLOCK:(k + 1) * BLOCK, :] for k in range(4))
        return cos_i * cos_b - sin_i * sin_b, sin_s * cos_b + cos_s * sin_b

    def rotated(x, cos, sin):
        swapped = jnp.where(first, pltpu.roll(x, 96, 1), pltpu.roll(x, 32, 1))
        return x * cos + swapped * sin

    local(w_kv, w_kv, 3).wait()
    w_qkv[:, q_width:] = w_kv[...].T
    w_second.wait()
    x_last(t).start()
    for load in w_rest:
        load.start()
    kv_loads[2].wait()
    q_load.wait()
    per_part = tok_rows // BLOCK
    for k in range(TOK_PARTS):
        tok_loads[k].wait()
        part = slice(k * tok_rows, (k + 1) * tok_rows)
        found = jnp.dot(tok[part, :], w_qkv[...], preferred_element_type=jnp.float32)
        qf[part, :] = found[:, :q_width]
        for b in range(per_part):
            i = k * per_part + b
            cos, sin = angle(i)
            x = found[b * BLOCK:(b + 1) * BLOCK, q_width:]
            turned = rotated(x, jnp.where(low, cos, 1.0), jnp.where(low, sin, 0.0))
            kv_own[i * BLOCK:(i + 1) * BLOCK, :] = turned.astype(jnp.bfloat16)

    def ends(sel, source):
        e = sel - source * blocks
        inside = (e >= 0) & (e < blocks)
        ef = e.astype(jnp.float32)
        lo = jnp.where(inside, ef, 1e6)
        hi = jnp.where(inside, ef, -1e6)
        lo = jnp.min(jnp.min(lo, axis=1, keepdims=True), axis=0, keepdims=True)
        hi = jnp.max(jnp.max(hi, axis=1, keepdims=True), axis=0, keepdims=True)
        return lo, hi

    r_iota = lax.broadcasted_iota(jnp.int32, (2 * BLOCK, rows), 0)
    c_iota = lax.broadcasted_iota(jnp.int32, (2 * BLOCK, rows), 1)
    r_in = lax.rem(r_iota, BLOCK).astype(jnp.float32)
    c_f = c_iota.astype(jnp.float32)

    def answer(dist):
        if dist >= n:
            return

        @pl.when(me + dist < n)
        def _():
            r = me + dist
            sel_copy(r, r).wait_recv()
            lo, hi = ends(sel_all[r], me)
            want = jnp.where(r_iota < BLOCK, lo, hi) * BLOCK + r_in
            pick = jnp.where(c_f == want, 1.0, 0.0).astype(jnp.bfloat16)
            chosen = jnp.dot(pick, kv_own[...], preferred_element_type=jnp.float32)
            send_kv[r] = chosen.astype(jnp.bfloat16)
            kv_copy(me, r).start()

    both = pl.ds(0, 2 * quarter)
    local(wo_h.at[both], wfull.at[t, both], 1).wait()
    own_copy(t).start()

    sel_f = sel_all[me].astype(jnp.float32)
    base = (me * blocks).astype(jnp.float32)
    local_id = (lax.broadcasted_iota(jnp.int32, (blocks, rows), 1) // BLOCK).astype(jnp.float32) + base
    hit = jnp.zeros((blocks, rows), jnp.float32)
    for k in range(topk):
        hit = jnp.where(sel_f[:, k:k + 1] == local_id, 1.0, hit)
    bias_l[...] = jnp.where(hit > 0.5, 0.0, NEG)

    slot = lax.broadcasted_iota(jnp.int32, (blocks, 2 * BLOCK), 1)
    for s in range(n - 1):
        lo, hi = ends(sel_all[me], s)
        ident = jnp.where(slot < BLOCK, lo, jnp.where(hi != lo, hi, -1e6)) + (s * blocks)
        hit = jnp.zeros((blocks, 2 * BLOCK), jnp.float32)
        for k in range(topk):
            hit = jnp.where(sel_f[:, k:k + 1] == ident, 1.0, hit)
        bias_r[s] = jnp.where((hit > 0.5) & (s < me), 0.0, NEG)

    def with_ones(kv):
        at = lax.broadcasted_iota(jnp.int32, kv.shape, 1)
        return jnp.where(at < HEAD_DIM, jnp.ones_like(kv), kv)

    q_row = lax.rem(lax.broadcasted_iota(jnp.int32, (group_rows, 128), 0), BLOCK)
    q_col = lax.broadcasted_iota(jnp.int32, (group_rows, 128), 1)
    zero = jnp.zeros((BLOCK, 128), jnp.float32)

    for i in range(blocks):
        cos, sin = angle(i)
        cos, sin = cos * HEAD_DIM ** -0.5, sin * HEAD_DIM ** -0.5
        stacked = []
        for pair in range(heads // 2):
            turned = rotated(qf[i * BLOCK:(i + 1) * BLOCK, pair * 128:(pair + 1) * 128], cos, sin)
            stacked.append(jnp.where(low, turned, zero))
            stacked.append(jnp.where(low, pltpu.roll(turned, HEAD_DIM, 1), zero))
        qs = jnp.concatenate(stacked, axis=0).astype(jnp.bfloat16)
        qs_s[i] = qs
        keys = 128 * (i // 2 + 1)
        kv = kv_own[:keys, :]
        scores = lax.dot_general(qs, kv, NT, preferred_element_type=jnp.float32)
        scores = scores + bias_l[i:i + 1, :keys]
        last = jnp.where(q_col <= q_row + (i % 2) * BLOCK, scores[:, keys - 128:], NEG)
        scores = last if keys == 128 else jnp.concatenate([scores[:, :keys - 128], last], axis=1)
        top = jnp.max(scores, axis=1, keepdims=True)
        p = jnp.exp(scores - top).astype(jnp.bfloat16)
        acc_s[i] = jnp.dot(p, with_ones(kv), preferred_element_type=jnp.float32)
        max_s[i] = jnp.broadcast_to(top, (group_rows, 128))
        for step, k in STEPS.get(i, ()):
            (pass_on, answer)[step](k)
    for dist in range(4, n):
        answer(dist)
    pass_late(0)

    for s in range(n - 1):
        @pl.when(s < me)
        def _():
            kv_copy(s, s).wait_recv()

    step = max(k for k in (1, 2, 3, 4) if (n - 1) % k == 0)

    def remote_part(at, i, count):
        kv = recv_kv[pl.ds(at, count)].reshape(count * 128, 128)
        scores = lax.dot_general(qs_s[i], kv, NT, preferred_element_type=jnp.float32)
        scores = jnp.concatenate(
            [scores[:, k * 128:(k + 1) * 128] + bias_r[at + k, pl.ds(i, 1), :] for k in range(count)], axis=1
        )
        before = max_s[i]
        top = jnp.maximum(before[:, :1], jnp.max(scores, axis=1, keepdims=True))
        p = jnp.exp(scores - top).astype(jnp.bfloat16)
        acc_s[i] = acc_s[i] * jnp.exp(before - top) + jnp.dot(
            p, with_ones(kv), preferred_element_type=jnp.float32
        )
        if n - 1 > step:
            max_s[i] = jnp.broadcast_to(top, (group_rows, 128))

    def remote_parts(many):
        if n - 1 > step:
            @pl.when(me > 0)
            def _():
                for i in many:
                    lax.fori_loop(0, (n - 1) // step, lambda at, _: (remote_part(at * step, i, step), 0)[1], 0)
        else:
            for count in range(1, n):
                @pl.when(me == count)
                def _():
                    for i in many:
                        remote_part(0, i, count)

    pass_on(4)
    per = blocks // n_tp

    def att_copy(owner, to, k):
        return remote(att.at[to], att_in.at[owner], a_ss, a_rs.at[k], "tp", to)

    far_near = lax.rem(near + n_tp // 2, n_tp)
    for turn, d in enumerate((far, far_near, near, t)):
        remote_parts([d * per + b for b in range(per)])
        for b in range(per):
            i = d * per + b
            for pair in range(heads // 2):
                even = acc_s[i, (2 * pair) * BLOCK:(2 * pair + 1) * BLOCK, :]
                odd = acc_s[i, (2 * pair + 1) * BLOCK:(2 * pair + 2) * BLOCK, :]
                top = jnp.where(low, pltpu.roll(even, HEAD_DIM, 1), odd)
                bottom = jnp.where(low, even, pltpu.roll(odd, HEAD_DIM, 1))
                att[d, b * BLOCK:(b + 1) * BLOCK, pair * 128:(pair + 1) * 128] = (top / bottom).astype(jnp.bfloat16)
        if turn < n_tp - 1:
            att_copy(t, d, turn // 2).start()
        if turn < len(LATE) - 1:
            pass_late(turn + 1)
        if turn == 2:
            pass_x_last()

    pass_last()
    own_copy(near).wait_recv()
    att_copy(near, near, 1).wait_recv()
    span = 512
    spans = [slice(col, col + span) for col in range(0, o_ref.shape[1], span)]
    for cols in spans:
        total = jnp.dot(att[t], wfull[t, :, cols], preferred_element_type=jnp.float32)
        total_s[:, cols] = total + jnp.dot(att_in[near], wfull[near, :, cols], preferred_element_type=jnp.float32)

    remote(wfull.at[far_near], wfull.at[far_near], w_ss, near_rs, "tp", near).wait_recv()
    remote(att_in.at[:2], att_in.at[:2], a_ss, a_rs.at[0], "tp", near).wait_recv()
    for cols in spans:
        total = total_s[:, cols] + jnp.dot(att_in[far], wfull[far, :, cols], preferred_element_type=jnp.float32)
        total += jnp.dot(att_in[far_near], wfull[far_near, :, cols], preferred_element_type=jnp.float32)
        o_ref[:, cols] = total.astype(jnp.bfloat16)

    remote(wfull.at[:3], wfull.at[:3], w_ss, near_rs, "tp", near).wait_send()
    remote(att.at[:3], att.at[:3], a_ss, near_rs, "tp", near).wait_send()
    for k in range(1, n):
        @pl.when(me == k)
        def _():
            remote(sel_all.at[:k], sel_all.at[:k], sel_ss, sel_rs.at[0], "kv", beside).wait_send()

        @pl.when(me == n - 1 - k)
        def _():
            remote(send_kv.at[:k], send_kv.at[:k], kv_ss, kv_rs.at[0], "kv", beside).wait_send()


def solution(mesh):
    n, n_tp, n_grp = mesh.shape["kv"], mesh.shape["tp"], mesh.shape["grp"]
    assert n_tp == 4 and n_grp == 2 and n % 2 == 0

    def shards(tokens, w_query, w_key, w_value, w_out, selection):
        rows, depth = tokens.shape
        q_width, width = w_query.shape[1], w_out.shape[1]
        blocks, topk = selection.shape[1:]
        heads = q_width // HEAD_DIM
        table = tables(n * blocks)
        bf, f32 = jnp.bfloat16, jnp.float32
        hbm = pl.BlockSpec(memory_space=pl.ANY)
        vmem = pl.BlockSpec(memory_space=pltpu.VMEM)
        dma = pltpu.SemaphoreType.DMA
        out_rows = rows // n_tp
        return pl.pallas_call(
            functools.partial(kernel, n, n_tp, n_grp),
            out_shape=pltpu.VMEM((out_rows, width), bf),
            in_specs=[hbm] * 7,
            out_specs=vmem,
            scratch_shapes=[
                pltpu.VMEM(table.shape, f32),
                pltpu.VMEM((rows, depth), bf),
                pltpu.VMEM((depth, q_width + 2 * HEAD_DIM), bf),
                pltpu.VMEM((2 * HEAD_DIM, depth), bf),
                pltpu.VMEM((n_tp, q_width, width), bf),
                pltpu.VMEM((n, blocks, topk), jnp.int32),
                pltpu.VMEM((rows, q_width), f32),
                pltpu.VMEM((rows, 128), bf),
                pltpu.VMEM((n, 128, 128), bf),
                pltpu.VMEM((n - 1, 128, 128), bf),
                pltpu.VMEM((blocks, rows), f32),
                pltpu.VMEM((n - 1, blocks, 128), f32),
                pltpu.VMEM((blocks, heads * BLOCK, 128), f32),
                pltpu.VMEM((blocks, heads * BLOCK, 128), f32),
                pltpu.VMEM((blocks, heads * BLOCK, 128), bf),
                pltpu.VMEM((n_tp, out_rows, q_width), bf),
                pltpu.VMEM((n_tp, out_rows, q_width), bf),
                pltpu.VMEM((out_rows, width), f32),
                dma((6 + TOK_PARTS,)),
                dma, dma((n,)), dma, dma((n - 1,)),
                dma, dma((len(CUTS),)), dma((len(LATE) + 1,)), dma, dma, dma, dma((2,)),
            ],
            compiler_params=pltpu.CompilerParams(
                collective_id=0, has_side_effects=True, vmem_limit_bytes=60 * 1024 * 1024
            ),
        )(tokens, w_query, w_key.T, w_value.T, w_out, selection, table)

    placed = (
        P(("grp", "kv"), None),
        P(None, "tp"),
        P(None, "tp"),
        P(None, "tp"),
        P("tp", None),
        P("tp", ("grp", "kv"), None),
    )
    return jax.shard_map(
        shards, mesh=mesh, in_specs=placed, out_specs=P(("grp", "kv", "tp"), None), check_vma=False
    )
```
